32 devices in a mesh: kv: 8 (over z, y), tp: 4 (over x, core).
Axes of the slice: x: 2, y: 2, z: 4, core: 2. Of those that a mesh axis runs over, the one named last changes fastest.
Arguments:
- x_piece: bfloat16 [128, 2048], P('kv'), may hold values from -6 to 6
- x_decode: bfloat16 [8, 2048], P('kv'), may hold values from -6 to 6
- norm_gain: float32 [2048], replicated, may hold values from 0.1 to 1.9
- w_query: bfloat16 [2048, 1024], P(None, 'tp'), may hold values from -0.1875 to 0.1875
- w_key: bfloat16 [2048, 1024], P(None, 'tp'), may hold values from -0.1875 to 0.1875
- w_value: bfloat16 [2048, 1024], P(None, 'tp'), may hold values from -0.125 to 0.125
- w_out: bfloat16 [1024, 2048], P(None, 'tp'), may hold values from -0.1875 to 0.1875
- head_gain: float32 [128], replicated, may hold values from 0.1 to 1.9
- lambdas: float32 [8], P('tp'), may hold values from 0.3 to 0.8
- piece_keys: bfloat16 [4096, 8, 128], P('kv', 'tp'), may hold values from -300 to 300
- piece_values: bfloat16 [4096, 8, 128], P('kv', 'tp'), may hold values from -6 to 6
- cache_keys: bfloat16 [8, 2048, 8, 128], P('kv', None, 'tp'), may hold values from -300 to 300
- cache_values: bfloat16 [8, 2048, 8, 128], P('kv', None, 'tp'), may hold values from -6 to 6
- cache_lengths: int32 [8], P('kv'), may hold values from 1 to 2048, as said below
Outputs:
- piece_out: bfloat16 [128, 2048], P('kv', 'tp')
- decode_out: bfloat16 [8, 2048], P('kv', 'tp')
The draws below stay inside these ranges and needn't reach their ends.
Inputs may be any that keep to these rules, and one draw needn't show every extreme that they name: `cache_lengths`: some sequence has exactly 2048 filled slots.
All inputs are finite; a program needn't handle non-finite values.
Results may differ from the reference program's by a relative error of at most 0.013.
The reference program's roundings to bfloat16 on the way count: a program that leaves them out, or rounds other values in their place, can miss the bound.
Values may be sent and summed in bfloat16 or wider, within the bound.
A program may use at most 64 MiB of HBM per device.

```python
import jax
import jax.numpy as jnp
from jax import lax

D = 2048
HEADS = 8
DK = 64
DV = 128
DEC_LEN = 2048
PIECE = 128
PAST = 4096
DEC = 8


def drawn_keys(key, shape):
    base = jax.random.normal(jax.random.fold_in(key, 11), shape, jnp.float32) * 1.32
    return jnp.clip(base, -300.0, 300.0).astype(jnp.bfloat16)


def draw_piece_keys(key, part):
    return drawn_keys(jax.random.fold_in(key, 21), (PAST, HEADS, 2 * DK))


def draw_cache_keys(key, part):
    return drawn_keys(jax.random.fold_in(key, 22), (DEC, DEC_LEN, HEADS, 2 * DK))


def draw_cache_lengths(key, part):
    first = jax.random.randint(jax.random.fold_in(key, 31), (DEC,), 1, DEC_LEN + 1)
    second = jax.random.randint(jax.random.fold_in(key, 32), (DEC,), 1, DEC_LEN + 1)
    lengths = jnp.minimum(first, second)
    longest = jax.random.randint(jax.random.fold_in(key, 33), (), 0, DEC)
    return lengths.at[longest].set(DEC_LEN).astype(jnp.int32)


def shard_levels(key, shape, pieces, low, largest):
    factor_of = 1.0
    for dim, blocks in pieces:
        draws = jax.random.uniform(jax.random.fold_in(jax.random.fold_in(key, 6), dim), (blocks,), jnp.float32, low / len(pieces), largest / len(pieces))
        factor_of = factor_of * jnp.repeat(jnp.exp(draws), shape[dim] // blocks).reshape((-1,) + (1,) * (len(shape) - 1 - dim))
    return factor_of


def normal_values(own_key, dims, width, limit, pieces=(), held_as=jnp.bfloat16):
    factor_of = shard_levels(own_key, dims, pieces, -0.22, 0.18) if pieces else 1.0
    entries = jax.random.normal(own_key, dims, jnp.float32) * width * factor_of
    return jnp.minimum(jnp.maximum(entries, -limit), limit).astype(held_as)


def setup_inputs(seed: int = 0) -> dict:
    splits = jax.random.split(jax.random.key(seed), 15)
    return {
        "x_piece": normal_values(splits[0], (PIECE, D), 1.0, 6.0, ((0, 8),)),
        "x_decode": normal_values(splits[1], (DEC, D), 1.0, 6.0, ((0, 8),)),
        "norm_gain": jnp.clip(1.0 + 0.18 * jax.random.normal(splits[2], (D,), jnp.float32), 0.1, 1.9),
        "w_query": normal_values(splits[3], (D, HEADS * 2 * DK), (4 * D // 7) ** -0.5, 0.1875, ((1, 4),)),
        "w_key": normal_values(splits[4], (D, HEADS * 2 * DK), (4 * D // 7) ** -0.5, 0.1875, ((1, 4),)),
        "w_value": normal_values(splits[5], (D, HEADS * DV), D ** -0.5, 0.125, ((1, 4),)),
        "w_out": normal_values(splits[6], (HEADS * DV, D), (HEADS * DV) ** -0.5, 0.1875, ((1, 4),)),
        "head_gain": jnp.clip(1.0 + 0.18 * jax.random.normal(splits[7], (DV,), jnp.float32), 0.1, 1.9),
        "lambdas": jnp.clip(0.3 + 0.5 * jax.random.uniform(splits[8], (HEADS,), jnp.float32) ** shard_levels(splits[8], (HEADS,), ((0, 4),), -0.2, 0.2), 0.3, 0.8),
        "piece_keys": draw_piece_keys(jax.random.fold_in(splits[14], 71), 0),
        "piece_values": normal_values(splits[10], (PAST, HEADS, DV), 1.0, 6.0, ((0, 8), (1, 4))),
        "cache_keys": draw_cache_keys(jax.random.fold_in(splits[14], 71), 0),
        "cache_values": normal_values(splits[12], (DEC, DEC_LEN, HEADS, DV), 1.0, 6.0, ((0, 8), (2, 4))),
        "cache_lengths": draw_cache_lengths(jax.random.fold_in(splits[14], 71), 0),
    }


EPS = 1e-06

def project_rows(rows, norm_gain, w_query, w_key, w_value):
    values32 = rows.astype(jnp.float32)
    normed = (values32 * lax.rsqrt(lax.optimization_barrier(jnp.mean(values32 * values32, axis=-1, keepdims=True)) + EPS) * norm_gain).astype(jnp.bfloat16)
    count = rows.shape[0]
    queries = jnp.dot(normed, w_query, preferred_element_type=jnp.float32).astype(jnp.bfloat16).reshape(count, HEADS, 2 * DK)
    new_keys = jnp.dot(normed, w_key, preferred_element_type=jnp.float32).astype(jnp.bfloat16).reshape(count, HEADS, 2 * DK)
    new_values = jnp.dot(normed, w_value, preferred_element_type=jnp.float32).astype(jnp.bfloat16).reshape(count, HEADS, DV)
    return (queries, new_keys, new_values)

def head_norm(attended, head_gain):
    return (attended * lax.rsqrt(lax.optimization_barrier(jnp.mean(attended * attended, axis=-1, keepdims=True)) + EPS) * head_gain).astype(jnp.bfloat16)

def reference(x_piece, x_decode, norm_gain, w_query, w_key, w_value, w_out, head_gain, lambdas, piece_keys, piece_values, cache_keys, cache_values, cache_lengths):
    score_scale = 1.0 / DK ** 0.5
    piece_q, piece_k, piece_v = project_rows(x_piece, norm_gain, w_query, w_key, w_value)
    dec_q, dec_k, dec_v = project_rows(x_decode, norm_gain, w_query, w_key, w_value)
    keys_all = jnp.concatenate([piece_keys, piece_k], axis=0).transpose(1, 0, 2)
    values_all = jnp.concatenate([piece_values, piece_v], axis=0).transpose(1, 0, 2)
    key_index = jnp.arange(PAST + PIECE, dtype=jnp.int32)
    block_rows = 512 if PIECE % 512 == 0 else PIECE
    nblocks = PIECE // block_rows

    def one_head(inputs):
        head_q, head_k, head_v, weight_two = inputs
        blocks = head_q.reshape(nblocks, block_rows, 2 * DK)

        def one_block(binputs):
            query_block, block_start = binputs
            query_pos = block_start + jnp.arange(block_rows, dtype=jnp.int32)
            allowed = (key_index[None, :] < PAST) | (key_index[None, :] - PAST <= query_pos[:, None])
            results = []
            for which_map in range(2):
                lower = which_map * DK
                scores = jnp.dot(query_block[:, lower:lower + DK], head_k[:, lower:lower + DK].T, preferred_element_type=jnp.float32) * score_scale
                scores = jnp.where(allowed, scores, -jnp.inf)
                row_max = lax.optimization_barrier(jnp.max(scores, axis=-1, keepdims=True))
                weights = jnp.exp(scores - row_max)
                totals = lax.optimization_barrier(jnp.sum(weights, axis=-1, keepdims=True))
                mixed = jnp.dot(weights.astype(jnp.bfloat16), head_v, preferred_element_type=jnp.float32)
                results.append(mixed / totals)
            return results[0] - weight_two * results[1]
        starts = jnp.arange(nblocks, dtype=jnp.int32) * block_rows
        return lax.map(one_block, (blocks, starts)).reshape(PIECE, DV)
    piece_att = lax.map(one_head, (piece_q.transpose(1, 0, 2), keys_all, values_all, lambdas))
    piece_att = piece_att.transpose(1, 0, 2)
    slot_index = jnp.arange(DEC_LEN + 1, dtype=jnp.int32)

    def one_sequence(inputs):
        seq_q, seq_k, seq_v, own_k, own_v, length = inputs
        keys = jnp.concatenate([seq_k, own_k[None]], axis=0).astype(jnp.float32)
        values = jnp.concatenate([seq_v, own_v[None]], axis=0).astype(jnp.float32)
        allowed = (slot_index < length) | (slot_index == DEC_LEN)
        query32 = seq_q.astype(jnp.float32)
        results = []
        for which_map in range(2):
            lower = which_map * DK
            scores = jnp.einsum('hd,khd->hk', query32[:, lower:lower + DK], keys[:, :, lower:lower + DK]) * score_scale
            scores = jnp.where(allowed[None, :], scores, -jnp.inf)
            row_max = lax.optimization_barrier(jnp.max(scores, axis=-1, keepdims=True))
            weights = jnp.exp(scores - row_max)
            totals = lax.optimization_barrier(jnp.sum(weights, axis=-1, keepdims=True))
            mixed = jnp.einsum('hk,khd->hd', weights.astype(jnp.bfloat16).astype(jnp.float32), values)
            results.append(mixed / totals)
        return results[0] - lambdas[:, None] * results[1]
    dec_att = lax.map(one_sequence, (dec_q, cache_keys, cache_values, dec_k, dec_v, cache_lengths))
    piece_heads = head_norm(piece_att, head_gain).reshape(PIECE, HEADS * DV)
    dec_heads = head_norm(dec_att, head_gain).reshape(DEC, HEADS * DV)
    piece_out = jnp.dot(piece_heads, w_out, preferred_element_type=jnp.float32).astype(jnp.bfloat16)
    decode_out = jnp.dot(dec_heads, w_out, preferred_element_type=jnp.float32).astype(jnp.bfloat16)
    return (piece_out, decode_out)
```

```python
import functools
import math

import jax
import jax.numpy as jnp
from jax import lax
from jax.experimental import pallas as pl
from jax.experimental.pallas import tpu as pltpu
from jax.sharding import PartitionSpec as P

EPS = 1e-06
MESH = pl.DeviceIdType.MESH
F32 = jnp.float32
BF16 = jnp.bfloat16
PAD = 16
LANES = 128
NEG = -jnp.inf


def dot_t(a, b):
    return lax.dot_general(a, b, (((1,), (1,)), ((), ())), preferred_element_type=F32)


def iota(shape, axis):
    return lax.broadcasted_iota(jnp.int32, shape, axis)


def step_kernel(
    kv, tp, rows, seqs, heads, width, group,
    xp, xd, ng, wq, wk, wv, wo, hg, lam, pk, pv, ck, cv, ln,
    po, do,
    xp_v, wq_v, wk_v, wv_v, wo_v, pk_v, pv_v, ck_v, cv_v,
    nrm, kf, vf, kh, vh, knew, vnew, qbuf, sbuf, rbuf, hbuf,
    load_sem, q_send, q_recv, s_send, s_recv, d_send, d_recv, h_send, h_recv,
):
    half = width // 2
    hw = heads * width
    maps = 2 * heads
    scale = math.log2(math.e) / math.sqrt(half)
    me = lax.axis_index("kv")
    col = lax.axis_index("tp")
    total = rows + PAD * seqs
    cached = kh.shape[1]

    pairs = [
        (xp, xp_v), (wq, wq_v), (wk, wk_v), (wv, wv_v), (ck, ck_v), (cv, cv_v),
        (pk, pk_v), (pv, pv_v), (wo, wo_v),
    ]
    loads = [pltpu.make_async_copy(s, d, load_sem.at[i]) for i, (s, d) in enumerate(pairs)]
    for load in loads:
        load.start()
    l_xp, l_wq, l_wk, l_wv, l_ck, l_cv, l_pk, l_pv, l_wo = loads

    def kv_peer(d):
        return {"kv": lax.rem(me + d, kv)}

    def tp_peer(d):
        return {"tp": lax.rem(col + d, tp)}

    barrier = pltpu.get_barrier_semaphore()
    for d in range(1, kv):
        pl.semaphore_signal(barrier, inc=1, device_id=kv_peer(d), device_id_type=MESH)
    for d in range(1, tp):
        pl.semaphore_signal(barrier, inc=1, device_id=tp_peer(d), device_id_type=MESH)

    def q_copy(d):
        return pltpu.make_async_remote_copy(
            src_ref=qbuf.at[0], dst_ref=qbuf.at[kv - d],
            send_sem=q_send.at[d], recv_sem=q_recv.at[kv - d],
            device_id=kv_peer(d), device_id_type=MESH,
        )

    def s_copy(d):
        return pltpu.make_async_remote_copy(
            src_ref=sbuf.at[d], dst_ref=rbuf.at[kv - d],
            send_sem=s_send.at[d], recv_sem=s_recv.at[kv - d],
            device_id=kv_peer(d), device_id_type=MESH,
        )

    def h_copy(d, start, size, send, recv):
        return pltpu.make_async_remote_copy(
            src_ref=hbuf.at[0, pl.ds(start, size)], dst_ref=hbuf.at[tp - d, pl.ds(start, size)],
            send_sem=send.at[d], recv_sem=recv.at[tp - d],
            device_id=tp_peer(d), device_id_type=MESH,
        )

    def norm_rows(x, gain):
        x32 = x.astype(F32)
        return x32 * lax.rsqrt(jnp.mean(x32 * x32, axis=-1, keepdims=True) + EPS) * gain

    gain = ng[...]
    for b in range(seqs):
        one = norm_rows(xd[pl.ds(b, 1), :], gain)
        nrm[pl.ds(rows + PAD * b, PAD), :] = jnp.broadcast_to(one, (PAD, one.shape[1])).astype(BF16)
    l_xp.wait()
    nrm[pl.ds(0, rows), :] = norm_rows(xp_v[...], gain).astype(BF16)
    l_wq.wait()
    q = jnp.dot(nrm[...], wq_v[...], preferred_element_type=F32).astype(BF16)
    qbuf[0] = q[:rows]
    pl.semaphore_wait(barrier, kv - 1 + tp - 1)
    for d in range(1, kv):
        q_copy(d).start()

    l_wk.wait()
    kn = jnp.dot(nrm[...], wk_v[...], preferred_element_type=F32).astype(BF16)
    l_wv.wait()
    vn = jnp.dot(nrm[...], wv_v[...], preferred_element_type=F32).astype(BF16)
    zeros = jnp.zeros((LANES - rows, width), BF16)
    for h in range(heads):
        knew[h, pl.ds(0, rows), :] = kn[:rows, h * width : (h + 1) * width]
        vnew[h, pl.ds(0, rows), :] = vn[:rows, h * width : (h + 1) * width]
        knew[h, pl.ds(rows, LANES - rows), :] = zeros
        vnew[h, pl.ds(rows, LANES - rows), :] = zeros

    l_ck.wait()
    l_cv.wait()
    head_gain = hg[...]

    def head_norm(att):
        return (
            att * lax.rsqrt(jnp.mean(att * att, axis=-1, keepdims=True) + EPS) * head_gain
        ).astype(BF16)

    slots = ck_v.shape[0] // seqs
    for b in range(seqs):
        first = rows + PAD * b
        row_head = iota((PAD, width), 0) // 2
        row_map = iota((PAD, width), 0) % 2
        lane_map = iota((PAD, width), 1) // half

        def pick(block):
            wide = block[first : first + PAD].astype(F32)
            out = wide[:, :width]
            for h in range(1, heads):
                out = jnp.where(row_head == h, wide[:, h * width : (h + 1) * width], out)
            return out

        q_rows = jnp.where(row_map == lane_map, pick(q), 0.0)
        s = dot_t(q_rows.astype(BF16), ck_v[pl.ds(b * slots, slots), :])
        key = iota(s.shape, 1)
        ok = (key // heads < ln[b]) & (key % heads == iota(s.shape, 0) // 2)
        s = jnp.where(ok, s, NEG)
        own = jnp.sum(q_rows * pick(kn), axis=-1, keepdims=True)
        top = jnp.maximum(jnp.max(s, axis=-1, keepdims=True), own)
        w = jnp.exp2((s - top) * scale)
        w_own = jnp.exp2((own - top) * scale)
        tot = jnp.sum(w, axis=-1, keepdims=True) + w_own
        mixed = jnp.dot(
            w.astype(BF16), cv_v[pl.ds(b * slots, slots), :], preferred_element_type=F32
        )
        mixed = (mixed + w_own.astype(BF16).astype(F32) * pick(vn)) / tot
        for h in range(heads):
            att = mixed[2 * h : 2 * h + 1] - lam[h] * mixed[2 * h + 1 : 2 * h + 2]
            hbuf[0, pl.ds(first, PAD), pl.ds(h * width, width)] = jnp.broadcast_to(
                head_norm(att), (PAD, width)
            )
    for d in range(1, tp):
        h_copy(d, rows, PAD * seqs, d_send, d_recv).start()

    l_pk.wait()
    kf[...] = pk_v[...].astype(F32)
    for h in range(heads):
        kh[h] = kf[pl.ds(h, cached, stride=heads), :].astype(BF16)
    l_pv.wait()
    vf[...] = pv_v[...].astype(F32)
    for h in range(heads):
        vh[h] = vf[pl.ds(h, cached, stride=heads), :].astype(BF16)

    span = group * rows
    lane_low = (iota((span, width), 1) < half).astype(F32)
    low = lane_low.astype(BF16)
    high = (1.0 - lane_low).astype(BF16)

    def attend(c):
        block = qbuf[pl.ds(c * group, group)].reshape(span, hw)
        place = iota((2 * span, LANES), 0) % span
        owner = place // rows + (me + c * group)
        owner = jnp.where(owner >= kv, owner - kv, owner)
        lane = iota((2 * span, LANES), 1)
        ok = (lane < rows) & (lane + me * rows <= owner * rows + place % rows)
        lane = iota((span, LANES), 1)
        kind = lane % (2 * maps)
        stats = jnp.zeros((span, LANES), F32)
        for h in range(heads):
            qh = block[:, h * width : (h + 1) * width]
            q2 = jnp.concatenate([qh * low, qh * high], axis=0)
            s1 = dot_t(q2, kh[h])
            s2 = jnp.where(ok, dot_t(q2, knew[h]), NEG)
            top = jnp.maximum(
                jnp.max(s1, axis=-1, keepdims=True), jnp.max(s2, axis=-1, keepdims=True)
            )
            w1 = jnp.exp2((s1 - top) * scale)
            w2 = jnp.exp2((s2 - top) * scale)
            tot = jnp.sum(w1, axis=-1, keepdims=True) + jnp.sum(w2, axis=-1, keepdims=True)
            mixed = jnp.dot(w1.astype(BF16), vh[h], preferred_element_type=F32) + jnp.dot(
                w2.astype(BF16), vnew[h], preferred_element_type=F32
            )
            mixed = mixed.astype(BF16)
            for m in range(2):
                at = 2 * h + m
                part = slice(m * span, (m + 1) * span)
                sbuf[pl.ds(c * group, group), pl.ds(at * rows, rows), :] = mixed[part].reshape(
                    group, rows, width
                )
                stats = jnp.where(kind == at, top[part], stats)
                stats = jnp.where(kind == maps + at, tot[part], stats)
        hi = stats.astype(BF16).astype(F32)
        rest = stats - hi
        mid = rest.astype(BF16).astype(F32)
        lo = rest - mid
        piece = lane // (2 * maps)
        packed = jnp.where(piece == 0, hi, jnp.where(piece == 1, mid, lo)).astype(BF16)
        sbuf[pl.ds(c * group, group), pl.ds(maps * rows, rows), :] = packed.reshape(
            group, rows, LANES
        )

    for d in range(1, kv):
        q_copy(d).wait_recv()
    chunks = kv // group
    if chunks == 1:
        attend(0)
    else:
        lax.fori_loop(0, chunks, lambda c, carry: (attend(c), carry)[1], 0)
    for d in range(1, kv):
        s_copy(d).start()
    rbuf[0] = sbuf[0]
    l_wo.wait()
    for d in range(1, kv):
        s_copy(d).wait_recv()

    stats = rbuf[:, pl.ds(maps * rows, rows), :].astype(F32).reshape(kv * rows, LANES)
    step = 2 * maps
    stats = stats + pltpu.roll(stats, LANES - step, 1) + pltpu.roll(stats, LANES - 2 * step, 1)
    tots = pltpu.roll(stats, LANES - maps, 1)
    top = stats[:rows]
    for p in range(1, kv):
        top = jnp.maximum(top, stats[p * rows : (p + 1) * rows])
    factors = []
    tot = jnp.zeros((rows, LANES), F32)
    for p in range(kv):
        part = slice(p * rows, (p + 1) * rows)
        factors.append(jnp.exp2((stats[part] - top) * scale))
        tot = tot + factors[p] * tots[part]
    lane = iota((rows, LANES), 1)
    sign = jnp.ones((rows, LANES), F32)
    for h in range(heads):
        sign = jnp.where(lane == 2 * h + 1, -lam[h], sign)
    inverse = sign / tot
    atts = [jnp.zeros((rows, width), F32) for _ in range(heads)]
    for p in range(kv):
        coef = factors[p] * inverse
        for at in range(maps):
            atts[at // 2] = atts[at // 2] + coef[:, at : at + 1] * rbuf[
                p, pl.ds(at * rows, rows), :
            ].astype(F32)
    for h in range(heads):
        hbuf[0, pl.ds(0, rows), pl.ds(h * width, width)] = head_norm(atts[h])
    for d in range(1, tp):
        h_copy(d, 0, rows, h_send, h_recv).start()

    def out_part(s):
        start = pl.multiple_of(lax.rem(col + s, tp) * hw, hw)
        return jnp.dot(hbuf[s], wo_v[pl.ds(start, hw), :], preferred_element_type=F32)

    acc = out_part(0)
    for d in range(1, tp):
        h_copy(tp - d, rows, PAD * seqs, d_send, d_recv).wait_recv()
        h_copy(tp - d, 0, rows, h_send, h_recv).wait_recv()
        acc = acc + out_part(d)
    po[...] = acc[:rows].astype(BF16)
    for b in range(seqs):
        do[pl.ds(b, 1), :] = acc[rows + PAD * b : rows + PAD * b + 1].astype(BF16)
    for d in range(1, kv):
        q_copy(d).wait_send()
        s_copy(d).wait_send()
    for d in range(1, tp):
        h_copy(d, rows, PAD * seqs, d_send, d_recv).wait_send()
        h_copy(d, 0, rows, h_send, h_recv).wait_send()


def shards(
    x_piece,
    x_decode,
    norm_gain,
    w_query,
    w_key,
    w_value,
    w_out,
    head_gain,
    lambdas,
    piece_keys,
    piece_values,
    cache_keys,
    cache_values,
    cache_lengths,
):
    rows, d_model = x_piece.shape
    seqs = x_decode.shape[0]
    heads = lambdas.shape[0]
    cached, _, width = piece_keys.shape
    slots = cache_keys.shape[1]
    kv = lax.axis_size("kv")
    tp = lax.axis_size("tp")
    hw = heads * width
    features = w_out.shape[1]
    total = rows + PAD * seqs
    group = max(1, min(kv, 128 // rows))
    any_spec = pl.BlockSpec(memory_space=pl.ANY)
    vmem = pl.BlockSpec(memory_space=pltpu.VMEM)
    smem = pl.BlockSpec(memory_space=pltpu.SMEM)
    dma = pltpu.SemaphoreType.DMA
    message = (2 * heads + 1) * rows
    scratch = [
        pltpu.VMEM((rows, d_model), BF16),
        pltpu.VMEM((d_model, hw), BF16),
        pltpu.VMEM((d_model, hw), BF16),
        pltpu.VMEM((d_model, hw), BF16),
        pltpu.VMEM(w_out.shape, BF16),
        pltpu.VMEM((cached * heads, width), BF16),
        pltpu.VMEM((cached * heads, width), BF16),
        pltpu.VMEM((seqs * slots * heads, width), BF16),
        pltpu.VMEM((seqs * slots * heads, width), BF16),
        pltpu.VMEM((total, d_model), BF16),
        pltpu.VMEM((cached * heads, width), F32),
        pltpu.VMEM((cached * heads, width), F32),
        pltpu.VMEM((heads, cached, width), BF16),
        pltpu.VMEM((heads, cached, width), BF16),
        pltpu.VMEM((heads, LANES, width), BF16),
        pltpu.VMEM((heads, LANES, width), BF16),
        pltpu.VMEM((kv, rows, hw), BF16),
        pltpu.VMEM((kv, message, width), BF16),
        pltpu.VMEM((kv, message, width), BF16),
        pltpu.VMEM((tp, total, hw), BF16),
        dma((9,)),
        dma((kv,)),
        dma((kv,)),
        dma((kv,)),
        dma((kv,)),
        dma((tp,)),
        dma((tp,)),
        dma((tp,)),
        dma((tp,)),
    ]
    return pl.pallas_call(
        functools.partial(step_kernel, kv, tp, rows, seqs, heads, width, group),
        out_shape=(
            jax.ShapeDtypeStruct((rows, features), BF16),
            jax.ShapeDtypeStruct((seqs, features), BF16),
        ),
        in_specs=[
            any_spec, vmem, vmem, any_spec, any_spec, any_spec, any_spec, vmem, smem,
            any_spec, any_spec, any_spec, any_spec, smem,
        ],
        out_specs=(vmem, vmem),
        scratch_shapes=scratch,
        compiler_params=pltpu.CompilerParams(collective_id=0, has_side_effects=True),
        name="step",
    )(
        x_piece,
        x_decode,
        norm_gain.reshape(1, d_model),
        w_query,
        w_key,
        w_value,
        w_out,
        head_gain.reshape(1, width),
        lambdas,
        piece_keys.reshape(cached * heads, width),
        piece_values.reshape(cached * heads, width),
        cache_keys.reshape(seqs * slots * heads, width),
        cache_values.reshape(seqs * slots * heads, width),
        cache_lengths,
    )


def solution(mesh):
    placed = (
        P("kv", None),
        P("kv", None),
        P(),
        P(None, "tp"),
        P(None, "tp"),
        P(None, "tp"),
        P(None, "tp"),
        P(),
        P("tp"),
        P("kv", "tp", None),
        P("kv", "tp", None),
        P("kv", None, "tp", None),
        P("kv", None, "tp", None),
        P("kv"),
    )
    return jax.shard_map(
        shards,
        mesh=mesh,
        in_specs=placed,
        out_specs=(P("kv", "tp"), P("kv", "tp")),
        check_vma=False,
    )
```

```python
import functools
import math

import jax
import jax.numpy as jnp
from jax import lax
from jax.experimental import pallas as pl
from jax.experimental.pallas import tpu as pltpu
from jax.sharding import PartitionSpec as P

EPS = 1e-06
MESH = pl.DeviceIdType.MESH
F32 = jnp.float32
BF16 = jnp.bfloat16
PAD = 16
LANES = 128
NEG = -jnp.inf


def dot_t(a, b):
    return lax.dot_general(a, b, (((1,), (1,)), ((), ())), preferred_element_type=F32)


def iota(shape, axis):
    return lax.broadcasted_iota(jnp.int32, shape, axis)


def step_kernel(
    kv, tp, rows, seqs, heads, width, group,
    xp, xd, ng, wq, wk, wv, wo, hg, lam, pk, pv, ck, cv, ln,
    po, do,
    xp_v, xd_v, ng_v, hg_v, lam_s, ln_s, wq_v, wk_v, wv_v, wo_v, pk_v, pv_v, ck_v, cv_v,
    nrm, kf, vf, kh, vh, knew, vnew, qbuf, sbuf, rbuf, hbuf,
    load_sem, q_send, q_recv, s_send, s_recv, d_send, d_recv, h_send, h_recv,
):
    half = width // 2
    hw = heads * width
    maps = 2 * heads
    scale = math.log2(math.e) / math.sqrt(half)
    me = lax.axis_index("kv")
    col = lax.axis_index("tp")
    cached = kh.shape[1]

    pairs = [
        (xp, xp_v), (ng, ng_v), (xd, xd_v), (wq, wq_v), (lam, lam_s), (ln, ln_s), (hg, hg_v),
        (wk, wk_v), (wv, wv_v), (ck, ck_v), (cv, cv_v), (pk, pk_v), (pv, pv_v), (wo, wo_v),
    ]
    loads = [pltpu.make_async_copy(s, d, load_sem.at[i]) for i, (s, d) in enumerate(pairs)]
    for load in loads:
        load.start()
    l_xp, l_ng, l_xd, l_wq, l_lam, l_ln, l_hg, l_wk, l_wv, l_ck, l_cv, l_pk, l_pv, l_wo = loads

    bits = kv.bit_length() - 1
    paired = kv == 1 << bits

    def partner(d):
        if not paired:
            return lax.rem(me + d, kv)
        out = 0
        for b in range(bits):
            mine = lax.rem(lax.div(me, 1 << b), 2)
            if isinstance(d, int):
                out = out + (1 << b) * ((1 - mine) if (d >> b) & 1 else mine)
            else:
                out = out + (1 << b) * lax.rem(mine + lax.rem(lax.div(d, 1 << b), 2), 2)
        return out

    def kv_peer(d):
        return {"kv": partner(d)}

    def back(d):
        return d if paired else kv - d

    def tp_peer(d):
        return {"tp": lax.rem(col + d, tp)}

    barrier = pltpu.get_barrier_semaphore()
    for d in range(kv - 1, 0, -1):
        pl.semaphore_signal(barrier, inc=1, device_id=kv_peer(d), device_id_type=MESH)
    for d in range(1, tp):
        pl.semaphore_signal(barrier, inc=1, device_id=tp_peer(d), device_id_type=MESH)

    def q_copy(d):
        return pltpu.make_async_remote_copy(
            src_ref=qbuf.at[0], dst_ref=qbuf.at[back(d)],
            send_sem=q_send.at[d], recv_sem=q_recv.at[back(d)],
            device_id=kv_peer(d), device_id_type=MESH,
        )

    def s_copy(d):
        return pltpu.make_async_remote_copy(
            src_ref=sbuf.at[d], dst_ref=rbuf.at[back(d)],
            send_sem=s_send.at[d], recv_sem=s_recv.at[back(d)],
            device_id=kv_peer(d), device_id_type=MESH,
        )

    def h_copy(d, start, size, send, recv):
        return pltpu.make_async_remote_copy(
            src_ref=hbuf.at[0, pl.ds(start, size)], dst_ref=hbuf.at[tp - d, pl.ds(start, size)],
            send_sem=send.at[d], recv_sem=recv.at[tp - d],
            device_id=tp_peer(d), device_id_type=MESH,
        )

    def norm_rows(x, gain):
        x32 = x.astype(F32)
        return x32 * lax.rsqrt(jnp.mean(x32 * x32, axis=-1, keepdims=True) + EPS) * gain

    l_xp.wait()
    l_ng.wait()
    gain = ng_v[...]
    nrm[pl.ds(0, rows), :] = norm_rows(xp_v[...], gain).astype(BF16)
    l_xd.wait()
    for b in range(seqs):
        one = norm_rows(xd_v[pl.ds(b, 1), :], gain)
        nrm[pl.ds(rows + PAD * b, PAD), :] = jnp.broadcast_to(one, (PAD, one.shape[1])).astype(BF16)
    l_wq.wait()
    q = jnp.dot(nrm[...], wq_v[...], preferred_element_type=F32).astype(BF16)
    qbuf[0] = q[:rows]
    pl.semaphore_wait(barrier, kv - 1 + tp - 1)
    for d in range(kv - 1, 0, -1):
        q_copy(d).start()

    l_wk.wait()
    kn = jnp.dot(nrm[...], wk_v[...], preferred_element_type=F32).astype(BF16)
    l_wv.wait()
    vn = jnp.dot(nrm[...], wv_v[...], preferred_element_type=F32).astype(BF16)
    zeros = jnp.zeros((LANES - rows, width), BF16)
    for h in range(heads):
        knew[h, pl.ds(0, rows), :] = kn[:rows, h * width : (h + 1) * width]
        vnew[h, pl.ds(0, rows), :] = vn[:rows, h * width : (h + 1) * width]
        knew[h, pl.ds(rows, LANES - rows), :] = zeros
        vnew[h, pl.ds(rows, LANES - rows), :] = zeros

    l_ck.wait()
    l_cv.wait()
    l_hg.wait()
    l_lam.wait()
    l_ln.wait()
    head_gain = hg_v[...]

    def head_norm(att):
        return (
            att * lax.rsqrt(jnp.mean(att * att, axis=-1, keepdims=True) + EPS) * head_gain
        ).astype(BF16)

    slots = ck_v.shape[0] // seqs
    for b in range(seqs):
        first = rows + PAD * b
        row_head = iota((PAD, width), 0) // 2
        row_map = iota((PAD, width), 0) % 2
        lane_map = iota((PAD, width), 1) // half

        def pick(block):
            wide = block[first : first + PAD].astype(F32)
            out = wide[:, :width]
            for h in range(1, heads):
                out = jnp.where(row_head == h, wide[:, h * width : (h + 1) * width], out)
            return out

        q_rows = jnp.where(row_map == lane_map, pick(q), 0.0)
        s = dot_t(q_rows.astype(BF16), ck_v[pl.ds(b * slots, slots), :])
        key = iota(s.shape, 1)
        ok = (key // heads < ln_s[b]) & (key % heads == iota(s.shape, 0) // 2)
        s = jnp.where(ok, s, NEG)
        own = jnp.sum(q_rows * pick(kn), axis=-1, keepdims=True)
        top = jnp.maximum(jnp.max(s, axis=-1, keepdims=True), own)
        w = jnp.exp2((s - top) * scale)
        w_own = jnp.exp2((own - top) * scale)
        tot = jnp.sum(w, axis=-1, keepdims=True) + w_own
        mixed = jnp.dot(
            w.astype(BF16), cv_v[pl.ds(b * slots, slots), :], preferred_element_type=F32
        )
        mixed = (mixed + w_own.astype(BF16).astype(F32) * pick(vn)) / tot
        for h in range(heads):
            att = mixed[2 * h : 2 * h + 1] - lam_s[h] * mixed[2 * h + 1 : 2 * h + 2]
            hbuf[0, pl.ds(first, PAD), pl.ds(h * width, width)] = jnp.broadcast_to(
                head_norm(att), (PAD, width)
            )
    for d in range(1, tp):
        h_copy(d, rows, PAD * seqs, d_send, d_recv).start()

    l_pk.wait()
    kf[...] = pk_v[...].astype(F32)
    for h in range(heads):
        kh[h] = kf[pl.ds(h, cached, stride=heads), :].astype(BF16)
    l_pv.wait()
    vf[...] = pv_v[...].astype(F32)
    for h in range(heads):
        vh[h] = vf[pl.ds(h, cached, stride=heads), :].astype(BF16)

    span = group * rows
    lane_low = (iota((span, width), 1) < half).astype(F32)
    low = lane_low.astype(BF16)
    high = (1.0 - lane_low).astype(BF16)

    def attend(c):
        block = qbuf[pl.ds(c * group, group)].reshape(span, hw)
        place = iota((2 * span, LANES), 0) % span
        slot = place // rows
        ahead = place % rows
        for g in range(group):
            ahead = jnp.where(slot == g, ahead + (partner(c * group + g) - me) * rows, ahead)
        lane = iota((2 * span, LANES), 1)
        ok = (lane < rows) & (lane <= ahead)
        lane = iota((span, LANES), 1)
        kind = lane % (2 * maps)
        stats = jnp.zeros((span, LANES), F32)
        for h in range(heads):
            qh = block[:, h * width : (h + 1) * width]
            q2 = jnp.concatenate([qh * low, qh * high], axis=0)
            s1 = dot_t(q2, kh[h])
            s2 = jnp.where(ok, dot_t(q2, knew[h]), NEG)
            top = jnp.maximum(
                jnp.max(s1, axis=-1, keepdims=True), jnp.max(s2, axis=-1, keepdims=True)
            )
            w1 = jnp.exp2((s1 - top) * scale)
            w2 = jnp.exp2((s2 - top) * scale)
            tot = jnp.sum(w1, axis=-1, keepdims=True) + jnp.sum(w2, axis=-1, keepdims=True)
            mixed = jnp.dot(w1.astype(BF16), vh[h], preferred_element_type=F32) + jnp.dot(
                w2.astype(BF16), vnew[h], preferred_element_type=F32
            )
            mixed = mixed.astype(BF16)
            for m in range(2):
                at = 2 * h + m
                part = slice(m * span, (m + 1) * span)
                sbuf[pl.ds(c * group, group), pl.ds(at * rows, rows), :] = mixed[part].reshape(
                    group, rows, width
                )
                stats = jnp.where(kind == at, top[part], stats)
                stats = jnp.where(kind == maps + at, tot[part], stats)
        hi = stats.astype(BF16).astype(F32)
        rest = stats - hi
        mid = rest.astype(BF16).astype(F32)
        lo = rest - mid
        piece = lane // (2 * maps)
        packed = jnp.where(piece == 0, hi, jnp.where(piece == 1, mid, lo)).astype(BF16)
        sbuf[pl.ds(c * group, group), pl.ds(maps * rows, rows), :] = packed.reshape(
            group, rows, LANES
        )

    chunks = kv // group
    if chunks <= 2:
        for c in range(chunks):
            members = range(max(1, c * group), (c + 1) * group)
            for d in members:
                q_copy(d).wait_recv()
            attend(c)
            for d in members:
                s_copy(d).start()
    else:
        for d in range(1, kv):
            q_copy(d).wait_recv()
        lax.fori_loop(0, chunks, lambda c, carry: (attend(c), carry)[1], 0)
        for d in range(1, kv):
            s_copy(d).start()
    rbuf[0] = sbuf[0]
    l_wo.wait()
    for d in range(1, kv):
        s_copy(d).wait_recv()

    stats = rbuf[:, pl.ds(maps * rows, rows), :].astype(F32).reshape(kv * rows, LANES)
    step = 2 * maps
    stats = stats + pltpu.roll(stats, LANES - step, 1) + pltpu.roll(stats, LANES - 2 * step, 1)
    tots = pltpu.roll(stats, LANES - maps, 1)
    top = stats[:rows]
    for p in range(1, kv):
        top = jnp.maximum(top, stats[p * rows : (p + 1) * rows])
    factors = []
    tot = jnp.zeros((rows, LANES), F32)
    for p in range(kv):
        part = slice(p * rows, (p + 1) * rows)
        factors.append(jnp.exp2((stats[part] - top) * scale))
        tot = tot + factors[p] * tots[part]
    lane = iota((rows, LANES), 1)
    sign = jnp.ones((rows, LANES), F32)
    for h in range(heads):
        sign = jnp.where(lane == 2 * h + 1, -lam_s[h], sign)
    inverse = sign / tot
    atts = [jnp.zeros((rows, width), F32) for _ in range(heads)]
    for p in range(kv):
        coef = factors[p] * inverse
        for at in range(maps):
            atts[at // 2] = atts[at // 2] + coef[:, at : at + 1] * rbuf[
                p, pl.ds(at * rows, rows), :
            ].astype(F32)
    for h in range(heads):
        hbuf[0, pl.ds(0, rows), pl.ds(h * width, width)] = head_norm(atts[h])
    for d in range(1, tp):
        h_copy(d, 0, rows, h_send, h_recv).start()

    def out_part(s):
        start = pl.multiple_of(lax.rem(col + s, tp) * hw, hw)
        return jnp.dot(hbuf[s], wo_v[pl.ds(start, hw), :], preferred_element_type=F32)

    acc = out_part(0)
    for d in range(1, tp):
        h_copy(tp - d, rows, PAD * seqs, d_send, d_recv).wait_recv()
        h_copy(tp - d, 0, rows, h_send, h_recv).wait_recv()
        acc = acc + out_part(d)
    po[...] = acc[:rows].astype(BF16)
    for b in range(seqs):
        do[pl.ds(b, 1), :] = acc[rows + PAD * b : rows + PAD * b + 1].astype(BF16)
    for d in range(1, kv):
        q_copy(d).wait_send()
        s_copy(d).wait_send()
    for d in range(1, tp):
        h_copy(d, rows, PAD * seqs, d_send, d_recv).wait_send()
        h_copy(d, 0, rows, h_send, h_recv).wait_send()


def shards(
    x_piece,
    x_decode,
    norm_gain,
    w_query,
    w_key,
    w_value,
    w_out,
    head_gain,
    lambdas,
    piece_keys,
    piece_values,
    cache_keys,
    cache_values,
    cache_lengths,
):
    rows, d_model = x_piece.shape
    seqs = x_decode.shape[0]
    heads = lambdas.shape[0]
    cached, _, width = piece_keys.shape
    slots = cache_keys.shape[1]
    kv = lax.axis_size("kv")
    tp = lax.axis_size("tp")
    hw = heads * width
    features = w_out.shape[1]
    total = rows + PAD * seqs
    group = max(1, min(kv // 2, 128 // rows))
    hbm = pl.BlockSpec(memory_space=pltpu.HBM)
    vmem = pl.BlockSpec(memory_space=pltpu.VMEM)
    dma = pltpu.SemaphoreType.DMA
    message = (2 * heads + 1) * rows
    scratch = [
        pltpu.VMEM((rows, d_model), BF16),
        pltpu.VMEM((seqs, d_model), BF16),
        pltpu.VMEM((1, d_model), F32),
        pltpu.VMEM((1, width), F32),
        pltpu.SMEM((heads,), F32),
        pltpu.SMEM((seqs,), jnp.int32),
        pltpu.VMEM((d_model, hw), BF16),
        pltpu.VMEM((d_model, hw), BF16),
        pltpu.VMEM((d_model, hw), BF16),
        pltpu.VMEM(w_out.shape, BF16),
        pltpu.VMEM((cached * heads, width), BF16),
        pltpu.VMEM((cached * heads, width), BF16),
        pltpu.VMEM((seqs * slots * heads, width), BF16),
        pltpu.VMEM((seqs * slots * heads, width), BF16),
        pltpu.VMEM((total, d_model), BF16),
        pltpu.VMEM((cached * heads, width), F32),
        pltpu.VMEM((cached * heads, width), F32),
        pltpu.VMEM((heads, cached, width), BF16),
        pltpu.VMEM((heads, cached, width), BF16),
        pltpu.VMEM((heads, LANES, width), BF16),
        pltpu.VMEM((heads, LANES, width), BF16),
        pltpu.VMEM((kv, rows, hw), BF16),
        pltpu.VMEM((kv, message, width), BF16),
        pltpu.VMEM((kv, message, width), BF16),
        pltpu.VMEM((tp, total, hw), BF16),
        dma((14,)),
        dma((kv,)),
        dma((kv,)),
        dma((kv,)),
        dma((kv,)),
        dma((tp,)),
        dma((tp,)),
        dma((tp,)),
        dma((tp,)),
    ]
    return pl.pallas_call(
        functools.partial(step_kernel, kv, tp, rows, seqs, heads, width, group),
        out_shape=(
            pltpu.VMEM((rows, features), BF16),
            pltpu.VMEM((seqs, features), BF16),
        ),
        in_specs=[hbm] * 14,
        out_specs=(vmem, vmem),
        scratch_shapes=scratch,
        compiler_params=pltpu.CompilerParams(collective_id=0, has_side_effects=True),
        name="step",
    )(
        x_piece,
        x_decode,
        norm_gain.reshape(1, d_model),
        w_query,
        w_key,
        w_value,
        w_out,
        head_gain.reshape(1, width),
        lambdas,
        piece_keys.reshape(cached * heads, width),
        piece_values.reshape(cached * heads, width),
        cache_keys.reshape(seqs * slots * heads, width),
        cache_values.reshape(seqs * slots * heads, width),
        cache_lengths,
    )


def solution(mesh):
    placed = (
        P("kv", None),
        P("kv", None),
        P(),
        P(None, "tp"),
        P(None, "tp"),
        P(None, "tp"),
        P(None, "tp"),
        P(),
        P("tp"),
        P("kv", "tp", None),
        P("kv", "tp", None),
        P("kv", None, "tp", None),
        P("kv", None, "tp", None),
        P("kv"),
    )
    return jax.shard_map(
        shards,
        mesh=mesh,
        in_specs=placed,
        out_specs=(P("kv", "tp"), P("kv", "tp")),
        check_vma=False,
    )
```

```python
import functools
import math

import jax
import jax.numpy as jnp
from jax import lax
from jax.experimental import pallas as pl
from jax.experimental.pallas import tpu as pltpu
from jax.sharding import PartitionSpec as P

EPS = 1e-06
MESH = pl.DeviceIdType.MESH
F32 = jnp.float32
BF16 = jnp.bfloat16
PAD = 16
LANES = 128
NEG = -jnp.inf


def dot_t(a, b):
    return lax.dot_general(a, b, (((1,), (1,)), ((), ())), preferred_element_type=F32)


def iota(shape, axis):
    return lax.broadcasted_iota(jnp.int32, shape, axis)


def step_kernel(
    kv, tp, rows, seqs, heads, width, group,
    xp, xd, ng, wq, wk, wv, wo, hg, lam, pk, pv, ck, cv, ln,
    po, do,
    xp_v, xd_v, ng_v, hg_v, lam_s, ln_s, wq_v, wk_v, wv_v, wo_v, pk_v, pv_v, ck_v, cv_v,
    nrm, kf, vf, kh, vh, knew, vnew, qbuf, sbuf, rbuf, hbuf,
    load_sem, q_send, q_recv, s_send, s_recv, d_send, d_recv, h_send, h_recv,
):
    half = width // 2
    hw = heads * width
    maps = 2 * heads
    scale = math.log2(math.e) / math.sqrt(half)
    me = lax.axis_index("kv")
    col = lax.axis_index("tp")
    cached = kh.shape[1]

    pairs = [
        (xp, xp_v), (ng, ng_v), (xd, xd_v), (wq, wq_v), (lam, lam_s), (ln, ln_s), (hg, hg_v),
        (wk, wk_v), (wv, wv_v), (ck, ck_v), (cv, cv_v), (pk, pk_v), (pv, pv_v), (wo, wo_v),
    ]
    loads = [pltpu.make_async_copy(s, d, load_sem.at[i]) for i, (s, d) in enumerate(pairs)]
    for load in loads[:4]:
        load.start()
    l_xp, l_ng, l_xd, l_wq, l_lam, l_ln, l_hg, l_wk, l_wv, l_ck, l_cv, l_pk, l_pv, l_wo = loads

    bits = kv.bit_length() - 1
    paired = kv == 1 << bits

    def partner(d):
        if not paired:
            return lax.rem(me + d, kv)
        out = 0
        for b in range(bits):
            mine = lax.rem(lax.div(me, 1 << b), 2)
            if isinstance(d, int):
                out = out + (1 << b) * ((1 - mine) if (d >> b) & 1 else mine)
            else:
                out = out + (1 << b) * lax.rem(mine + lax.rem(lax.div(d, 1 << b), 2), 2)
        return out

    def kv_peer(d):
        return {"kv": partner(d)}

    def back(d):
        return d if paired else kv - d

    def tp_peer(d):
        return {"tp": lax.rem(col + d, tp)}

    barrier = pltpu.get_barrier_semaphore()
    for d in range(kv - 1, 0, -1):
        pl.semaphore_signal(barrier, inc=1, device_id=kv_peer(d), device_id_type=MESH)
    for d in range(1, tp):
        pl.semaphore_signal(barrier, inc=1, device_id=tp_peer(d), device_id_type=MESH)

    def q_copy(d):
        return pltpu.make_async_remote_copy(
            src_ref=qbuf.at[0], dst_ref=qbuf.at[back(d)],
            send_sem=q_send.at[d], recv_sem=q_recv.at[back(d)],
            device_id=kv_peer(d), device_id_type=MESH,
        )

    message = sbuf.shape[1]

    def s_copy(d, start=0, size=message):
        return pltpu.make_async_remote_copy(
            src_ref=sbuf.at[d, pl.ds(start, size)],
            dst_ref=rbuf.at[back(d), pl.ds(start, size)],
            send_sem=s_send.at[d], recv_sem=s_recv.at[back(d)],
            device_id=kv_peer(d), device_id_type=MESH,
        )

    def h_copy(d, start, size, send, recv):
        return pltpu.make_async_remote_copy(
            src_ref=hbuf.at[0, pl.ds(start, size)], dst_ref=hbuf.at[tp - d, pl.ds(start, size)],
            send_sem=send.at[d], recv_sem=recv.at[tp - d],
            device_id=tp_peer(d), device_id_type=MESH,
        )

    def norm_rows(x, gain):
        x32 = x.astype(F32)
        return x32 * lax.rsqrt(jnp.mean(x32 * x32, axis=-1, keepdims=True) + EPS) * gain

    l_xp.wait()
    for load in loads[4:]:
        load.start()
    l_ng.wait()
    gain = ng_v[...]
    nrm[pl.ds(0, rows), :] = norm_rows(xp_v[...], gain).astype(BF16)
    l_xd.wait()
    for b in range(seqs):
        one = norm_rows(xd_v[pl.ds(b, 1), :], gain)
        nrm[pl.ds(rows + PAD * b, PAD), :] = jnp.broadcast_to(one, (PAD, one.shape[1])).astype(BF16)
    l_wq.wait()
    q = jnp.dot(nrm[...], wq_v[...], preferred_element_type=F32).astype(BF16)
    qbuf[0] = q[:rows]
    pl.semaphore_wait(barrier, kv - 1 + tp - 1)
    for d in range(kv - 1, 0, -1):
        q_copy(d).start()

    l_wk.wait()
    kn = jnp.dot(nrm[...], wk_v[...], preferred_element_type=F32).astype(BF16)
    l_wv.wait()
    vn = jnp.dot(nrm[...], wv_v[...], preferred_element_type=F32).astype(BF16)
    zeros = jnp.zeros((LANES - rows, width), BF16)
    for h in range(heads):
        knew[h, pl.ds(0, rows), :] = kn[:rows, h * width : (h + 1) * width]
        vnew[h, pl.ds(0, rows), :] = vn[:rows, h * width : (h + 1) * width]
        knew[h, pl.ds(rows, LANES - rows), :] = zeros
        vnew[h, pl.ds(rows, LANES - rows), :] = zeros

    l_ck.wait()
    l_cv.wait()
    l_hg.wait()
    l_lam.wait()
    l_ln.wait()
    head_gain = hg_v[...]

    def head_norm(att):
        return (
            att * lax.rsqrt(jnp.mean(att * att, axis=-1, keepdims=True) + EPS) * head_gain
        ).astype(BF16)

    slots = ck_v.shape[0] // seqs
    for b in range(seqs):
        first = rows + PAD * b
        row_head = iota((PAD, width), 0) // 2
        row_map = iota((PAD, width), 0) % 2
        lane_map = iota((PAD, width), 1) // half

        def pick(block):
            wide = block[first : first + PAD].astype(F32)
            out = wide[:, :width]
            for h in range(1, heads):
                out = jnp.where(row_head == h, wide[:, h * width : (h + 1) * width], out)
            return out

        q_rows = jnp.where(row_map == lane_map, pick(q), 0.0)
        s = dot_t(q_rows.astype(BF16), ck_v[pl.ds(b * slots, slots), :])
        key = iota(s.shape, 1)
        ok = (key // heads < ln_s[b]) & (key % heads == iota(s.shape, 0) // 2)
        s = jnp.where(ok, s, NEG)
        own = jnp.sum(q_rows * pick(kn), axis=-1, keepdims=True)
        top = jnp.maximum(jnp.max(s, axis=-1, keepdims=True), own)
        w = jnp.exp2((s - top) * scale)
        w_own = jnp.exp2((own - top) * scale)
        tot = jnp.sum(w, axis=-1, keepdims=True) + w_own
        mixed = jnp.dot(
            w.astype(BF16), cv_v[pl.ds(b * slots, slots), :], preferred_element_type=F32
        )
        mixed = (mixed + w_own.astype(BF16).astype(F32) * pick(vn)) / tot
        for h in range(heads):
            att = mixed[2 * h : 2 * h + 1] - lam_s[h] * mixed[2 * h + 1 : 2 * h + 2]
            hbuf[0, pl.ds(first, PAD), pl.ds(h * width, width)] = jnp.broadcast_to(
                head_norm(att), (PAD, width)
            )
    for d in range(1, tp):
        h_copy(d, rows, PAD * seqs, d_send, d_recv).start()

    l_pk.wait()
    kf[...] = pk_v[...].astype(F32)
    for h in range(heads):
        kh[h] = kf[pl.ds(h, cached, stride=heads), :].astype(BF16)
    l_pv.wait()
    vf[...] = pv_v[...].astype(F32)
    for h in range(heads):
        vh[h] = vf[pl.ds(h, cached, stride=heads), :].astype(BF16)

    span = group * rows
    lane_low = (iota((span, width), 1) < half).astype(F32)
    low = lane_low.astype(BF16)
    high = (1.0 - lane_low).astype(BF16)

    def attend(c, members=()):
        block = qbuf[pl.ds(c * group, group)].reshape(span, hw)
        place = iota((2 * span, LANES), 0) % span
        slot = place // rows
        ahead = place % rows
        for g in range(group):
            ahead = jnp.where(slot == g, ahead + (partner(c * group + g) - me) * rows, ahead)
        lane = iota((2 * span, LANES), 1)
        ok = (lane < rows) & (lane <= ahead)
        lane = iota((span, LANES), 1)
        kind = lane % (2 * maps)
        stats = jnp.zeros((span, LANES), F32)
        for h in range(heads):
            qh = block[:, h * width : (h + 1) * width]
            q2 = jnp.concatenate([qh * low, qh * high], axis=0)
            s1 = dot_t(q2, kh[h])
            s2 = jnp.where(ok, dot_t(q2, knew[h]), NEG)
            top = jnp.maximum(
                jnp.max(s1, axis=-1, keepdims=True), jnp.max(s2, axis=-1, keepdims=True)
            )
            w1 = jnp.exp2((s1 - top) * scale)
            w2 = jnp.exp2((s2 - top) * scale)
            tot = jnp.sum(w1, axis=-1, keepdims=True) + jnp.sum(w2, axis=-1, keepdims=True)
            mixed = jnp.dot(w1.astype(BF16), vh[h], preferred_element_type=F32) + jnp.dot(
                w2.astype(BF16), vnew[h], preferred_element_type=F32
            )
            mixed = mixed.astype(BF16)
            for m in range(2):
                at = 2 * h + m
                part = slice(m * span, (m + 1) * span)
                sbuf[pl.ds(c * group, group), pl.ds(at * rows, rows), :] = mixed[part].reshape(
                    group, rows, width
                )
                stats = jnp.where(kind == at, top[part], stats)
                stats = jnp.where(kind == maps + at, tot[part], stats)
            if h < heads - 1:
                for d in members:
                    s_copy(d, 2 * h * rows, 2 * rows).start()
        hi = stats.astype(BF16).astype(F32)
        rest = stats - hi
        mid = rest.astype(BF16).astype(F32)
        lo = rest - mid
        piece = lane // (2 * maps)
        packed = jnp.where(piece == 0, hi, jnp.where(piece == 1, mid, lo)).astype(BF16)
        sbuf[pl.ds(c * group, group), pl.ds(maps * rows, rows), :] = packed.reshape(
            group, rows, LANES
        )
        for d in members:
            s_copy(d, 2 * (heads - 1) * rows, 3 * rows).start()

    chunks = kv // group
    if chunks <= 2:
        for c in range(chunks):
            members = range((c + 1) * group - 1, max(1, c * group) - 1, -1)
            for d in members:
                q_copy(d).wait_recv()
            attend(c, members)
    else:
        for d in range(1, kv):
            q_copy(d).wait_recv()
        lax.fori_loop(0, chunks, lambda c, carry: (attend(c), carry)[1], 0)
        for d in range(1, kv):
            s_copy(d).start()
    rbuf[0] = sbuf[0]
    l_wo.wait()
    for d in range(1, kv):
        s_copy(d).wait_recv()

    stats = rbuf[:, pl.ds(maps * rows, rows), :].astype(F32).reshape(kv * rows, LANES)
    step = 2 * maps
    stats = stats + pltpu.roll(stats, LANES - step, 1) + pltpu.roll(stats, LANES - 2 * step, 1)
    tots = pltpu.roll(stats, LANES - maps, 1)
    top = stats[:rows]
    for p in range(1, kv):
        top = jnp.maximum(top, stats[p * rows : (p + 1) * rows])
    factors = []
    tot = jnp.zeros((rows, LANES), F32)
    for p in range(kv):
        part = slice(p * rows, (p + 1) * rows)
        factors.append(jnp.exp2((stats[part] - top) * scale))
        tot = tot + factors[p] * tots[part]
    lane = iota((rows, LANES), 1)
    sign = jnp.ones((rows, LANES), F32)
    for h in range(heads):
        sign = jnp.where(lane == 2 * h + 1, -lam_s[h], sign)
    inverse = sign / tot
    atts = [jnp.zeros((rows, width), F32) for _ in range(heads)]
    for p in range(kv):
        coef = factors[p] * inverse
        for at in range(maps):
            atts[at // 2] = atts[at // 2] + coef[:, at : at + 1] * rbuf[
                p, pl.ds(at * rows, rows), :
            ].astype(F32)
    for h in range(heads):
        hbuf[0, pl.ds(0, rows), pl.ds(h * width, width)] = head_norm(atts[h])
    for d in range(1, tp):
        h_copy(d, 0, rows, h_send, h_recv).start()

    def out_part(s):
        start = pl.multiple_of(lax.rem(col + s, tp) * hw, hw)
        return jnp.dot(hbuf[s], wo_v[pl.ds(start, hw), :], preferred_element_type=F32)

    acc = out_part(0)
    for d in range(1, tp):
        h_copy(tp - d, rows, PAD * seqs, d_send, d_recv).wait_recv()
        h_copy(tp - d, 0, rows, h_send, h_recv).wait_recv()
        acc = acc + out_part(d)
    po[...] = acc[:rows].astype(BF16)
    for b in range(seqs):
        do[pl.ds(b, 1), :] = acc[rows + PAD * b : rows + PAD * b + 1].astype(BF16)
    for d in range(1, kv):
        q_copy(d).wait_send()
        s_copy(d).wait_send()
    for d in range(1, tp):
        h_copy(d, rows, PAD * seqs, d_send, d_recv).wait_send()
        h_copy(d, 0, rows, h_send, h_recv).wait_send()


def store_kernel(a, b, po, do, sem):
    copies = [pltpu.make_async_copy(a, po, sem.at[0]), pltpu.make_async_copy(b, do, sem.at[1])]
    for copy in copies:
        copy.start()
    for copy in copies:
        copy.wait()


def shards(
    x_piece,
    x_decode,
    norm_gain,
    w_query,
    w_key,
    w_value,
    w_out,
    head_gain,
    lambdas,
    piece_keys,
    piece_values,
    cache_keys,
    cache_values,
    cache_lengths,
):
    rows, d_model = x_piece.shape
    seqs = x_decode.shape[0]
    heads = lambdas.shape[0]
    cached, _, width = piece_keys.shape
    slots = cache_keys.shape[1]
    kv = lax.axis_size("kv")
    tp = lax.axis_size("tp")
    hw = heads * width
    features = w_out.shape[1]
    total = rows + PAD * seqs
    group = max(1, min(kv // 2, 128 // rows))
    hbm = pl.BlockSpec(memory_space=pltpu.HBM)
    vmem = pl.BlockSpec(memory_space=pltpu.VMEM)
    dma = pltpu.SemaphoreType.DMA
    message = (2 * heads + 1) * rows
    scratch = [
        pltpu.VMEM((rows, d_model), BF16),
        pltpu.VMEM((seqs, d_model), BF16),
        pltpu.VMEM((1, d_model), F32),
        pltpu.VMEM((1, width), F32),
        pltpu.SMEM((heads,), F32),
        pltpu.SMEM((seqs,), jnp.int32),
        pltpu.VMEM((d_model, hw), BF16),
        pltpu.VMEM((d_model, hw), BF16),
        pltpu.VMEM((d_model, hw), BF16),
        pltpu.VMEM(w_out.shape, BF16),
        pltpu.VMEM((cached * heads, width), BF16),
        pltpu.VMEM((cached * heads, width), BF16),
        pltpu.VMEM((seqs * slots * heads, width), BF16),
        pltpu.VMEM((seqs * slots * heads, width), BF16),
        pltpu.VMEM((total, d_model), BF16),
        pltpu.VMEM((cached * heads, width), F32),
        pltpu.VMEM((cached * heads, width), F32),
        pltpu.VMEM((heads, cached, width), BF16),
        pltpu.VMEM((heads, cached, width), BF16),
        pltpu.VMEM((heads, LANES, width), BF16),
        pltpu.VMEM((heads, LANES, width), BF16),
        pltpu.VMEM((kv, rows, hw), BF16),
        pltpu.VMEM((kv, message, width), BF16),
        pltpu.VMEM((kv, message, width), BF16),
        pltpu.VMEM((tp, total, hw), BF16),
        dma((14,)),
        dma((kv,)),
        dma((kv,)),
        dma((kv,)),
        dma((kv,)),
        dma((tp,)),
        dma((tp,)),
        dma((tp,)),
        dma((tp,)),
    ]
    held = pl.pallas_call(
        functools.partial(step_kernel, kv, tp, rows, seqs, heads, width, group),
        out_shape=(
            pltpu.VMEM((rows, features), BF16),
            pltpu.VMEM((seqs, features), BF16),
        ),
        in_specs=[hbm] * 14,
        out_specs=(vmem, vmem),
        scratch_shapes=scratch,
        compiler_params=pltpu.CompilerParams(collective_id=0, has_side_effects=True),
        name="step",
    )(
        x_piece,
        x_decode,
        norm_gain.reshape(1, d_model),
        w_query,
        w_key,
        w_value,
        w_out,
        head_gain.reshape(1, width),
        lambdas,
        piece_keys.reshape(cached * heads, width),
        piece_values.reshape(cached * heads, width),
        cache_keys.reshape(seqs * slots * heads, width),
        cache_values.reshape(seqs * slots * heads, width),
        cache_lengths,
    )
    return pl.pallas_call(
        store_kernel,
        out_shape=tuple(jax.ShapeDtypeStruct(a.shape, a.dtype) for a in held),
        in_specs=[vmem, vmem],
        out_specs=(hbm, hbm),
        scratch_shapes=[dma((2,))],
        name="store",
    )(*[pltpu.with_memory_space_constraint(a, pltpu.VMEM) for a in held])


def solution(mesh):
    placed = (
        P("kv", None),
        P("kv", None),
        P(),
        P(None, "tp"),
        P(None, "tp"),
        P(None, "tp"),
        P(None, "tp"),
        P(),
        P("tp"),
        P("kv", "tp", None),
        P("kv", "tp", None),
        P("kv", None, "tp", None),
        P("kv", None, "tp", None),
        P("kv"),
    )
    return jax.shard_map(
        shards,
        mesh=mesh,
        in_specs=placed,
        out_specs=(P("kv", "tp"), P("kv", "tp")),
        check_vma=False,
    )
```

```python
import functools
import math

import jax
import jax.numpy as jnp
from jax import lax
from jax.experimental import pallas as pl
from jax.experimental.pallas import tpu as pltpu
from jax.sharding import PartitionSpec as P

EPS = 1e-06
MESH = pl.DeviceIdType.MESH
F32 = jnp.float32
BF16 = jnp.bfloat16
PAD = 16
LANES = 128
NEG = -jnp.inf


def dot_t(a, b):
    return lax.dot_general(a, b, (((1,), (1,)), ((), ())), preferred_element_type=F32)


def iota(shape, axis):
    return lax.broadcasted_iota(jnp.int32, shape, axis)


def step_kernel(
    kv, tp, rows, seqs, heads, width, group,
    xp, xd, ng, wq, wk, wv, wo, hg, lam, pk, pv, ck, cv, ln,
    po, do,
    xp_v, xd_v, ng_v, hg_v, lam_s, ln_s, wq_v, wk_v, wv_v, wo_v, pk_v, pv_v, ck_v, cv_v,
    nrm, kf, vf, kh, vh, knew, vnew, qbuf, sbuf, rbuf, hbuf,
    load_sem, q_send, q_recv, s_send, s_recv, d_send, d_recv, h_send, h_recv,
):
    half = width // 2
    hw = heads * width
    maps = 2 * heads
    scale = math.log2(math.e) / math.sqrt(half)
    me = lax.axis_index("kv")
    col = lax.axis_index("tp")
    cached = kh.shape[1]

    pairs = [
        (xp, xp_v), (ng, ng_v), (xd, xd_v), (wq, wq_v), (lam, lam_s), (ln, ln_s), (hg, hg_v),
        (wk, wk_v), (wv, wv_v), (ck, ck_v), (cv, cv_v), (pk, pk_v), (pv, pv_v), (wo, wo_v),
    ]
    loads = [pltpu.make_async_copy(s, d, load_sem.at[i]) for i, (s, d) in enumerate(pairs)]
    for load in loads[:4]:
        load.start()
    l_xp, l_ng, l_xd, l_wq, l_lam, l_ln, l_hg, l_wk, l_wv, l_ck, l_cv, l_pk, l_pv, l_wo = loads

    bits = kv.bit_length() - 1
    paired = kv == 1 << bits

    def partner(d):
        if not paired:
            return lax.rem(me + d, kv)
        out = 0
        for b in range(bits):
            mine = lax.rem(lax.div(me, 1 << b), 2)
            if isinstance(d, int):
                out = out + (1 << b) * ((1 - mine) if (d >> b) & 1 else mine)
            else:
                out = out + (1 << b) * lax.rem(mine + lax.rem(lax.div(d, 1 << b), 2), 2)
        return out

    def kv_peer(d):
        return {"kv": partner(d)}

    def back(d):
        return d if paired else kv - d

    def tp_peer(d):
        return {"tp": lax.rem(col + d, tp)}

    barrier = pltpu.get_barrier_semaphore()
    for d in range(kv - 1, 0, -1):
        pl.semaphore_signal(barrier, inc=1, device_id=kv_peer(d), device_id_type=MESH)
    for d in range(1, tp):
        pl.semaphore_signal(barrier, inc=1, device_id=tp_peer(d), device_id_type=MESH)

    def q_copy(d):
        return pltpu.make_async_remote_copy(
            src_ref=qbuf.at[0], dst_ref=qbuf.at[back(d)],
            send_sem=q_send.at[d], recv_sem=q_recv.at[back(d)],
            device_id=kv_peer(d), device_id_type=MESH,
        )

    message = sbuf.shape[1]
    fold = rows // 2

    def s_copy(d, start=0, size=message):
        return pltpu.make_async_remote_copy(
            src_ref=sbuf.at[d, pl.ds(start, size)],
            dst_ref=rbuf.at[back(d), pl.ds(start, size)],
            send_sem=s_send.at[d], recv_sem=s_recv.at[back(d)],
            device_id=kv_peer(d), device_id_type=MESH,
        )

    def h_copy(d, start, size, send, recv):
        return pltpu.make_async_remote_copy(
            src_ref=hbuf.at[0, pl.ds(start, size)], dst_ref=hbuf.at[tp - d, pl.ds(start, size)],
            send_sem=send.at[d], recv_sem=recv.at[tp - d],
            device_id=tp_peer(d), device_id_type=MESH,
        )

    def norm_rows(x, gain):
        x32 = x.astype(F32)
        return x32 * lax.rsqrt(jnp.mean(x32 * x32, axis=-1, keepdims=True) + EPS) * gain

    l_xp.wait()
    for load in loads[4:]:
        load.start()
    l_ng.wait()
    gain = ng_v[...]
    nrm[pl.ds(0, rows), :] = norm_rows(xp_v[...], gain).astype(BF16)
    l_xd.wait()
    for b in range(seqs):
        one = norm_rows(xd_v[pl.ds(b, 1), :], gain)
        nrm[pl.ds(rows + PAD * b, PAD), :] = jnp.broadcast_to(one, (PAD, one.shape[1])).astype(BF16)
    l_wq.wait()
    q = jnp.dot(nrm[...], wq_v[...], preferred_element_type=F32).astype(BF16)
    qbuf[0] = q[:rows]
    pl.semaphore_wait(barrier, kv - 1 + tp - 1)
    for d in range(kv - 1, 0, -1):
        q_copy(d).start()

    l_wk.wait()
    kn = jnp.dot(nrm[...], wk_v[...], preferred_element_type=F32).astype(BF16)
    l_wv.wait()
    vn = jnp.dot(nrm[...], wv_v[...], preferred_element_type=F32).astype(BF16)
    zeros = jnp.zeros((LANES - rows, width), BF16)
    for h in range(heads):
        knew[h, pl.ds(0, rows), :] = kn[:rows, h * width : (h + 1) * width]
        vnew[h, pl.ds(0, rows), :] = vn[:rows, h * width : (h + 1) * width]
        knew[h, pl.ds(rows, LANES - rows), :] = zeros
        vnew[h, pl.ds(rows, LANES - rows), :] = zeros

    l_ck.wait()
    l_cv.wait()
    l_hg.wait()
    l_lam.wait()
    l_ln.wait()
    head_gain = hg_v[...]

    def head_norm(att):
        return (
            att * lax.rsqrt(jnp.mean(att * att, axis=-1, keepdims=True) + EPS) * head_gain
        ).astype(BF16)

    slots = ck_v.shape[0] // seqs
    for b in range(seqs):
        first = rows + PAD * b
        row_head = iota((PAD, width), 0) // 2
        row_map = iota((PAD, width), 0) % 2
        lane_map = iota((PAD, width), 1) // half

        def pick(block):
            wide = block[first : first + PAD].astype(F32)
            out = wide[:, :width]
            for h in range(1, heads):
                out = jnp.where(row_head == h, wide[:, h * width : (h + 1) * width], out)
            return out

        q_rows = jnp.where(row_map == lane_map, pick(q), 0.0)
        s = dot_t(q_rows.astype(BF16), ck_v[pl.ds(b * slots, slots), :])
        key = iota(s.shape, 1)
        ok = (key // heads < ln_s[b]) & (key % heads == iota(s.shape, 0) // 2)
        s = jnp.where(ok, s, NEG)
        own = jnp.sum(q_rows * pick(kn), axis=-1, keepdims=True)
        top = jnp.maximum(jnp.max(s, axis=-1, keepdims=True), own)
        w = jnp.exp2((s - top) * scale)
        w_own = jnp.exp2((own - top) * scale)
        tot = jnp.sum(w, axis=-1, keepdims=True) + w_own
        mixed = jnp.dot(
            w.astype(BF16), cv_v[pl.ds(b * slots, slots), :], preferred_element_type=F32
        )
        mixed = (mixed + w_own.astype(BF16).astype(F32) * pick(vn)) / tot
        for h in range(heads):
            att = mixed[2 * h : 2 * h + 1] - lam_s[h] * mixed[2 * h + 1 : 2 * h + 2]
            hbuf[0, pl.ds(first, PAD), pl.ds(h * width, width)] = jnp.broadcast_to(
                head_norm(att), (PAD, width)
            )
    for d in range(1, tp):
        h_copy(d, rows, PAD * seqs, d_send, d_recv).start()

    l_pk.wait()
    kf[...] = pk_v[...].astype(F32)
    for h in range(heads):
        kh[h] = kf[pl.ds(h, cached, stride=heads), :].astype(BF16)
    l_pv.wait()
    vf[...] = pv_v[...].astype(F32)
    for h in range(heads):
        vh[h] = vf[pl.ds(h, cached, stride=heads), :].astype(BF16)

    span = group * rows
    lane_low = (iota((span, width), 1) < half).astype(F32)
    low = lane_low.astype(BF16)
    high = (1.0 - lane_low).astype(BF16)

    def attend(c, members=()):
        block = qbuf[pl.ds(c * group, group)].reshape(span, hw)
        place = iota((2 * span, LANES), 0) % span
        slot = place // rows
        ahead = place % rows
        for g in range(group):
            ahead = jnp.where(slot == g, ahead + (partner(c * group + g) - me) * rows, ahead)
        lane = iota((2 * span, LANES), 1)
        ok = (lane < rows) & (lane <= ahead)
        lane = iota((span, LANES), 1)
        kind = lane % (2 * maps)
        stats = jnp.zeros((span, LANES), F32)
        for h in range(heads):
            qh = block[:, h * width : (h + 1) * width]
            q2 = jnp.concatenate([qh * low, qh * high], axis=0)
            s1 = dot_t(q2, kh[h])
            s2 = jnp.where(ok, dot_t(q2, knew[h]), NEG)
            top = jnp.maximum(
                jnp.max(s1, axis=-1, keepdims=True), jnp.max(s2, axis=-1, keepdims=True)
            )
            w1 = jnp.exp2((s1 - top) * scale)
            w2 = jnp.exp2((s2 - top) * scale)
            tot = jnp.sum(w1, axis=-1, keepdims=True) + jnp.sum(w2, axis=-1, keepdims=True)
            mixed = jnp.dot(w1.astype(BF16), vh[h], preferred_element_type=F32) + jnp.dot(
                w2.astype(BF16), vnew[h], preferred_element_type=F32
            )
            mixed = mixed.astype(BF16)
            for m in range(2):
                at = 2 * h + m
                part = slice(m * span, (m + 1) * span)
                sbuf[pl.ds(c * group, group), pl.ds(at * rows, rows), :] = mixed[part].reshape(
                    group, rows, width
                )
                stats = jnp.where(kind == at, top[part], stats)
                stats = jnp.where(kind == maps + at, tot[part], stats)
            if h < heads - 1:
                for d in members:
                    s_copy(d, 2 * h * rows, 2 * rows).start()
        hi = stats.astype(BF16).astype(F32)
        rest = stats - hi
        mid = rest.astype(BF16).astype(F32)
        lo = rest - mid
        piece = lane // (2 * maps)
        packed = jnp.where(piece == 0, hi, jnp.where(piece == 1, mid, lo))
        packed = jnp.where(piece < 3, packed, 0.0).reshape(group, 2, fold, LANES)
        upper = pltpu.roll(packed[:, 1].reshape(group * fold, LANES), LANES // 2, 1)
        sbuf[pl.ds(c * group, group), pl.ds(maps * rows, fold), :] = (
            packed[:, 0] + upper.reshape(group, fold, LANES)
        ).astype(BF16)
        for d in members:
            s_copy(d, 2 * (heads - 1) * rows, 2 * rows + fold).start()

    chunks = kv // group
    if chunks <= 2:
        for c in range(chunks):
            members = range((c + 1) * group - 1, max(1, c * group) - 1, -1)
            for d in members:
                q_copy(d).wait_recv()
            attend(c, members)
    else:
        for d in range(1, kv):
            q_copy(d).wait_recv()
        lax.fori_loop(0, chunks, lambda c, carry: (attend(c), carry)[1], 0)
        for d in range(1, kv):
            s_copy(d).start()
    rbuf[0] = sbuf[0]
    l_wo.wait()
    for d in range(1, kv):
        s_copy(d).wait_recv()

    lower = rbuf[:, pl.ds(maps * rows, fold), :].astype(F32)
    upper = pltpu.roll(lower.reshape(kv * fold, LANES), LANES // 2, 1)
    stats = jnp.concatenate([lower, upper.reshape(kv, fold, LANES)], axis=1)
    stats = stats.reshape(kv * rows, LANES)
    step = 2 * maps
    stats = stats + pltpu.roll(stats, LANES - step, 1) + pltpu.roll(stats, LANES - 2 * step, 1)
    tots = pltpu.roll(stats, LANES - maps, 1)
    top = stats[:rows]
    for p in range(1, kv):
        top = jnp.maximum(top, stats[p * rows : (p + 1) * rows])
    factors = []
    tot = jnp.zeros((rows, LANES), F32)
    for p in range(kv):
        part = slice(p * rows, (p + 1) * rows)
        factors.append(jnp.exp2((stats[part] - top) * scale))
        tot = tot + factors[p] * tots[part]
    lane = iota((rows, LANES), 1)
    sign = jnp.ones((rows, LANES), F32)
    for h in range(heads):
        sign = jnp.where(lane == 2 * h + 1, -lam_s[h], sign)
    inverse = sign / tot
    atts = [jnp.zeros((rows, width), F32) for _ in range(heads)]
    for p in range(kv):
        coef = factors[p] * inverse
        for at in range(maps):
            atts[at // 2] = atts[at // 2] + coef[:, at : at + 1] * rbuf[
                p, pl.ds(at * rows, rows), :
            ].astype(F32)
    for h in range(heads):
        hbuf[0, pl.ds(0, rows), pl.ds(h * width, width)] = head_norm(atts[h])
    for d in range(1, tp):
        h_copy(d, 0, rows, h_send, h_recv).start()

    def out_part(s):
        start = pl.multiple_of(lax.rem(col + s, tp) * hw, hw)
        return jnp.dot(hbuf[s], wo_v[pl.ds(start, hw), :], preferred_element_type=F32)

    acc = out_part(0)
    for d in range(1, tp):
        h_copy(tp - d, rows, PAD * seqs, d_send, d_recv).wait_recv()
        h_copy(tp - d, 0, rows, h_send, h_recv).wait_recv()
        acc = acc + out_part(d)
    po[...] = acc[:rows].astype(BF16)
    for b in range(seqs):
        do[pl.ds(b, 1), :] = acc[rows + PAD * b : rows + PAD * b + 1].astype(BF16)
    for d in range(1, kv):
        q_copy(d).wait_send()
        s_copy(d).wait_send()
    for d in range(1, tp):
        h_copy(d, rows, PAD * seqs, d_send, d_recv).wait_send()
        h_copy(d, 0, rows, h_send, h_recv).wait_send()


def store_kernel(a, b, po, do, sem):
    copies = [pltpu.make_async_copy(a, po, sem.at[0]), pltpu.make_async_copy(b, do, sem.at[1])]
    for copy in copies:
        copy.start()
    for copy in copies:
        copy.wait()


def shards(
    x_piece,
    x_decode,
    norm_gain,
    w_query,
    w_key,
    w_value,
    w_out,
    head_gain,
    lambdas,
    piece_keys,
    piece_values,
    cache_keys,
    cache_values,
    cache_lengths,
):
    rows, d_model = x_piece.shape
    seqs = x_decode.shape[0]
    heads = lambdas.shape[0]
    cached, _, width = piece_keys.shape
    slots = cache_keys.shape[1]
    kv = lax.axis_size("kv")
    tp = lax.axis_size("tp")
    hw = heads * width
    features = w_out.shape[1]
    total = rows + PAD * seqs
    group = max(1, min(kv // 2, 128 // rows))
    hbm = pl.BlockSpec(memory_space=pltpu.HBM)
    vmem = pl.BlockSpec(memory_space=pltpu.VMEM)
    dma = pltpu.SemaphoreType.DMA
    message = 2 * heads * rows + rows // 2
    scratch = [
        pltpu.VMEM((rows, d_model), BF16),
        pltpu.VMEM((seqs, d_model), BF16),
        pltpu.VMEM((1, d_model), F32),
        pltpu.VMEM((1, width), F32),
        pltpu.SMEM((heads,), F32),
        pltpu.SMEM((seqs,), jnp.int32),
        pltpu.VMEM((d_model, hw), BF16),
        pltpu.VMEM((d_model, hw), BF16),
        pltpu.VMEM((d_model, hw), BF16),
        pltpu.VMEM(w_out.shape, BF16),
        pltpu.VMEM((cached * heads, width), BF16),
        pltpu.VMEM((cached * heads, width), BF16),
        pltpu.VMEM((seqs * slots * heads, width), BF16),
        pltpu.VMEM((seqs * slots * heads, width), BF16),
        pltpu.VMEM((total, d_model), BF16),
        pltpu.VMEM((cached * heads, width), F32),
        pltpu.VMEM((cached * heads, width), F32),
        pltpu.VMEM((heads, cached, width), BF16),
        pltpu.VMEM((heads, cached, width), BF16),
        pltpu.VMEM((heads, LANES, width), BF16),
        pltpu.VMEM((heads, LANES, width), BF16),
        pltpu.VMEM((kv, rows, hw), BF16),
        pltpu.VMEM((kv, message, width), BF16),
        pltpu.VMEM((kv, message, width), BF16),
        pltpu.VMEM((tp, total, hw), BF16),
        dma((14,)),
        dma((kv,)),
        dma((kv,)),
        dma((kv,)),
        dma((kv,)),
        dma((tp,)),
        dma((tp,)),
        dma((tp,)),
        dma((tp,)),
    ]
    held = pl.pallas_call(
        functools.partial(step_kernel, kv, tp, rows, seqs, heads, width, group),
        out_shape=(
            pltpu.VMEM((rows, features), BF16),
            pltpu.VMEM((seqs, features), BF16),
        ),
        in_specs=[hbm] * 14,
        out_specs=(vmem, vmem),
        scratch_shapes=scratch,
        compiler_params=pltpu.CompilerParams(collective_id=0, has_side_effects=True),
        name="step",
    )(
        x_piece,
        x_decode,
        norm_gain.reshape(1, d_model),
        w_query,
        w_key,
        w_value,
        w_out,
        head_gain.reshape(1, width),
        lambdas,
        piece_keys.reshape(cached * heads, width),
        piece_values.reshape(cached * heads, width),
        cache_keys.reshape(seqs * slots * heads, width),
        cache_values.reshape(seqs * slots * heads, width),
        cache_lengths,
    )
    return pl.pallas_call(
        store_kernel,
        out_shape=tuple(jax.ShapeDtypeStruct(a.shape, a.dtype) for a in held),
        in_specs=[vmem, vmem],
        out_specs=(hbm, hbm),
        scratch_shapes=[dma((2,))],
        name="store",
    )(*[pltpu.with_memory_space_constraint(a, pltpu.VMEM) for a in held])


def solution(mesh):
    placed = (
        P("kv", None),
        P("kv", None),
        P(),
        P(None, "tp"),
        P(None, "tp"),
        P(None, "tp"),
        P(None, "tp"),
        P(),
        P("tp"),
        P("kv", "tp", None),
        P("kv", "tp", None),
        P("kv", None, "tp", None),
        P("kv", None, "tp", None),
        P("kv"),
    )
    return jax.shard_map(
        shards,
        mesh=mesh,
        in_specs=placed,
        out_specs=(P("kv", "tp"), P("kv", "tp")),
        check_vma=False,
    )
```
